32 devices in a mesh: sp: 8 (over z, y), tp: 4 (over x, core).
Axes of the slice: x: 2, y: 2, z: 4, core: 2. Of those that a mesh axis runs over, the one named last changes fastest.
Arguments:
- residual: bfloat16 [6144, 2048], P(('sp', 'tp')), may hold values from -6 to 6
- queries: bfloat16 [6144, 1024], P('sp', 'tp'), may hold values from -240 to 240
- keys: bfloat16 [6144, 256], P('sp', 'tp'), may hold values from -6 to 6
- values: bfloat16 [6144, 256], P('sp', 'tp'), may hold values from -18 to 18
- sinks: float32 [16], P('tp'), may hold values from 1 to 6
- out_weight: bfloat16 [1024, 2048], replicated, may hold values from -0.5625 to 0.5625
- norm_gain: float32 [2048], replicated, may hold values from 0.1 to 1.9
- gate_weight: bfloat16 [2048, 5632], P('sp', 'tp'), may hold values from -0.125 to 0.125
- up_weight: bfloat16 [2048, 5632], P('sp', 'tp'), may hold values from -0.125 to 0.125
- down_weight: bfloat16 [5632, 2048], P('tp', 'sp'), may hold values from -0.078125 to 0.078125
Outputs:
- layer_out: bfloat16 [6144, 2048], P(('sp', 'tp'))
The draws below stay inside these ranges and needn't reach their ends.
All inputs are finite; a program needn't handle non-finite values.
Results may differ from the reference program's by a relative error of at most 0.014.
Values may be sent and summed in bfloat16 or wider, within the bound.
A program may use at most 128 MiB of HBM per device.

```python
import jax
import jax.numpy as jnp
from jax import lax

D = 2048
FF = 5632
HEAD = 64
QH = 16
KVH = 4
WINDOW = 128
ATT = 1024
TOKENS = 6144
N_TP = 4


def drawn(key):
    key_query, key_keys = jax.random.split(jax.random.fold_in(key, 7), 2)
    queries = jnp.clip(jax.random.normal(key_query, (TOKENS, QH * HEAD), jnp.float32), -6.0, 6.0)
    keyset = jnp.clip(jax.random.normal(key_keys, (TOKENS, KVH * HEAD), jnp.float32), -6.0, 6.0)
    return (queries, keyset)


def draw_queries(key, part):
    return drawn(key)[0].astype(jnp.bfloat16)


def draw_keys(key, part):
    return drawn(key)[1].astype(jnp.bfloat16)


def steps_of(rng, extent, shards, least, largest):
    def one(axis_at, shards_of):
        draws = jax.random.uniform(jax.random.fold_in(jax.random.fold_in(rng, 6), axis_at), (shards_of,), jnp.float32, least / len(shards), largest / len(shards))
        return jnp.repeat(jnp.exp(draws), extent[axis_at] // shards_of).reshape((-1,) + (1,) * (len(extent) - axis_at - 1))

    loudness = one(*shards[0])
    for cut in shards[1:]:
        loudness = loudness * one(*cut)
    return loudness


def gaussian(own_key, extent, spread, bound, shards=(), dtype=jnp.bfloat16):
    values = spread * jax.random.normal(own_key, extent, jnp.float32)
    if shards:
        values = values * steps_of(own_key, extent, shards, -0.22, 0.18)
    return jnp.clip(values, -bound, bound).astype(dtype)


def setup_inputs(seed: int = 0) -> dict:
    splits = jax.random.split(jax.random.key(seed), 11)
    residual = gaussian(splits[0], (TOKENS, D), 1.0, 6.0, ((0, 32),))
    queries = draw_queries(jax.random.fold_in(splits[10], 71), 0)
    keys = draw_keys(jax.random.fold_in(splits[10], 71), 0)
    values = gaussian(splits[3], (TOKENS, KVH * HEAD), 3.0, 18.0, ((0, 8), (1, 4)))
    sinks = jnp.clip(1.0 + 5.0 * jax.random.uniform(splits[4], (QH,), jnp.float32) ** steps_of(splits[4], (QH,), ((0, 4),), -0.2, 0.2), 1.0, 6.0)
    out_weight = gaussian(splits[5], (ATT, D), (3.0 / ATT ** 0.5), 0.5625)
    norm_gain = jnp.clip(1.0 + 0.18 * jax.random.normal(splits[6], (D,), jnp.float32), 0.1, 1.9)
    gate_weight = gaussian(splits[7], (D, FF), D ** -0.5, 0.125, ((0, 8), (1, 4)))
    up_weight = gaussian(splits[8], (D, FF), D ** -0.5, 0.125, ((0, 8), (1, 4)))
    down_weight = gaussian(splits[9], (FF, D), FF ** -0.5, 0.078125, ((0, 4), (1, 8)))
    return {"residual": residual, "queries": queries, "keys": keys, "values": values, "sinks": sinks, "out_weight": out_weight, "norm_gain": norm_gain, "gate_weight": gate_weight, "up_weight": up_weight, "down_weight": down_weight}


def attend(queries, keys_ext, values_ext, sinks, block_base):
    rows = queries.shape[0]
    nblk = rows // WINDOW
    qheads = sinks.shape[0]
    kheads = keys_ext.shape[1] // HEAD
    group = qheads // kheads
    qblock = queries.reshape(nblk, WINDOW, kheads, group, HEAD).astype(jnp.float32)

    def band(arr):
        first = arr[:rows].reshape(nblk, WINDOW, kheads, HEAD)
        second = arr[WINDOW:].reshape(nblk, WINDOW, kheads, HEAD)
        return jnp.concatenate([first, second], axis=1).astype(jnp.float32)
    kband = band(keys_ext)
    vband = band(values_ext)
    score = jnp.einsum('nqhgd,nkhd->nhgqk', qblock, kband) * HEAD ** (-0.5)
    qidx = jnp.arange(WINDOW)[:, None]
    kidx = jnp.arange(2 * WINDOW)[None, :]
    rel = qidx + WINDOW - kidx
    valid = (rel >= 0) & (rel < WINDOW)
    blocks = block_base + jnp.arange(nblk)
    valid = valid[None] & ((blocks > 0)[:, None, None] | (kidx >= WINDOW)[None])
    score = jnp.where(valid[:, None, None], score, -jnp.inf)
    sink = sinks.astype(jnp.float32).reshape(kheads, group)[None, :, :, None]
    top = jnp.maximum(lax.optimization_barrier(jnp.max(score, axis=-1)), sink)
    expd = jnp.exp(score - top[..., None])
    denom = lax.optimization_barrier(jnp.sum(expd, axis=-1)) + jnp.exp(sink - top)
    weights = (expd / denom[..., None]).astype(jnp.bfloat16)
    result = jnp.einsum('nhgqk,nkhd->nqhgd', weights.astype(jnp.float32), vband)
    return result.reshape(rows, qheads * HEAD).astype(jnp.bfloat16)

def reference(residual, queries, keys, values, sinks, out_weight, norm_gain, gate_weight, up_weight, down_weight):
    padding = jnp.zeros((WINDOW, keys.shape[1]), jnp.bfloat16)
    keys_ext = jnp.concatenate([padding, keys], axis=0)
    values_ext = jnp.concatenate([padding, values], axis=0)
    attention = attend(queries, keys_ext, values_ext, sinks, 0)
    proj = jnp.dot(attention, out_weight, preferred_element_type=jnp.float32)
    mixed = (residual.astype(jnp.float32) + proj).astype(jnp.bfloat16)
    mixf = mixed.astype(jnp.float32)
    normed = (mixf * lax.rsqrt(lax.optimization_barrier(jnp.mean(mixf * mixf, axis=-1, keepdims=True)) + 1e-06) * norm_gain).astype(jnp.bfloat16)
    gate = jnp.dot(normed, gate_weight, preferred_element_type=jnp.float32)
    upper = jnp.dot(normed, up_weight, preferred_element_type=jnp.float32)
    hidden = (jax.nn.silu(gate) * upper).astype(jnp.bfloat16)
    share = FF // N_TP
    ffn = jnp.zeros((hidden.shape[0], D), jnp.float32)
    for index in range(N_TP):
        part_sum = jnp.dot(hidden[:, index * share:(index + 1) * share], down_weight[index * share:(index + 1) * share], preferred_element_type=jnp.float32)
        ffn = ffn + lax.optimization_barrier(part_sum.astype(jnp.bfloat16)).astype(jnp.float32)
    return (mixed.astype(jnp.float32) + ffn).astype(jnp.bfloat16)
```

```python
import functools

import jax
import jax.numpy as jnp
from jax import lax
from jax.experimental import pallas as pl
from jax.experimental.pallas import tpu as pltpu
from jax.sharding import PartitionSpec as P

HEAD = 64
WINDOW = 128


def passed_along(block, axis, distance):
    devices = range(lax.axis_size(axis))
    route = [(i - distance, i) for i in devices if i - distance in devices]
    return lax.ppermute(block, axis, route)


def attend(queries, keys_ext, values_ext, sinks, block_base):
    rows = queries.shape[0]
    nblk = rows // WINDOW
    qheads = sinks.shape[0]
    kheads = keys_ext.shape[1] // HEAD
    group = qheads // kheads
    qblock = queries.reshape(nblk, WINDOW, kheads, group, HEAD).astype(jnp.float32)

    def band(arr):
        first = arr[:rows].reshape(nblk, WINDOW, kheads, HEAD)
        second = arr[WINDOW:].reshape(nblk, WINDOW, kheads, HEAD)
        return jnp.concatenate([first, second], axis=1).astype(jnp.float32)

    kband = band(keys_ext)
    vband = band(values_ext)
    score = jnp.einsum("nqhgd,nkhd->nhgqk", qblock, kband) * HEAD ** (-0.5)
    qidx = jnp.arange(WINDOW)[:, None]
    kidx = jnp.arange(2 * WINDOW)[None, :]
    rel = qidx + WINDOW - kidx
    valid = (rel >= 0) & (rel < WINDOW)
    blocks = block_base + jnp.arange(nblk)
    valid = valid[None] & ((blocks > 0)[:, None, None] | (kidx >= WINDOW)[None])
    score = jnp.where(valid[:, None, None], score, -jnp.inf)
    sink = sinks.reshape(kheads, group)[None, :, :, None]
    top = jnp.maximum(jnp.max(score, axis=-1), sink)
    expd = jnp.exp(score - top[..., None])
    denom = jnp.sum(expd, axis=-1) + jnp.exp(sink - top)
    weights = (expd / denom[..., None]).astype(jnp.bfloat16)
    result = jnp.einsum("nhgqk,nkhd->nqhgd", weights.astype(jnp.float32), vband)
    return result.reshape(rows, qheads * HEAD).astype(jnp.bfloat16)


def shards(
    residual,
    queries,
    keys,
    values,
    sinks,
    out_weight,
    norm_gain,
    gate_weight,
    up_weight,
    down_weight,
):
    rows_dev = queries.shape[0]
    prev_keys, prev_values = passed_along((keys[-WINDOW:], values[-WINDOW:]), "sp", 1)
    keys_ext = jnp.concatenate([prev_keys, keys], axis=0)
    values_ext = jnp.concatenate([prev_values, values], axis=0)
    attention = attend(
        queries, keys_ext, values_ext, sinks, lax.axis_index("sp") * (rows_dev // WINDOW)
    )
    width = attention.shape[1]
    mine = lax.dynamic_slice_in_dim(out_weight, lax.axis_index("tp") * width, width, 0)
    proj = lax.psum_scatter(
        jnp.dot(attention, mine, preferred_element_type=jnp.float32).astype(jnp.bfloat16),
        "tp",
        scatter_dimension=0,
        tiled=True,
    ).astype(jnp.float32)
    mixed = (residual.astype(jnp.float32) + proj).astype(jnp.bfloat16)
    mixf = mixed.astype(jnp.float32)
    normed = (
        mixf * lax.rsqrt(jnp.mean(mixf * mixf, axis=-1, keepdims=True) + 1e-06) * norm_gain
    ).astype(jnp.bfloat16)
    normed_all = lax.all_gather(normed, "tp", axis=0, tiled=True)
    gate = jnp.dot(
        normed_all,
        lax.all_gather(gate_weight, "sp", axis=0, tiled=True),
        preferred_element_type=jnp.float32,
    )
    upper = jnp.dot(
        normed_all,
        lax.all_gather(up_weight, "sp", axis=0, tiled=True),
        preferred_element_type=jnp.float32,
    )
    hidden = (jax.nn.silu(gate) * upper).astype(jnp.bfloat16)
    terms = jnp.dot(
        hidden,
        lax.all_gather(down_weight, "sp", axis=1, tiled=True),
        preferred_element_type=jnp.float32,
    )
    ffn = lax.psum_scatter(
        terms.astype(jnp.bfloat16), "tp", scatter_dimension=0, tiled=True
    ).astype(jnp.float32)
    return (mixed.astype(jnp.float32) + ffn).astype(jnp.bfloat16)


MESH = pl.DeviceIdType.MESH
F32 = jnp.float32
BF16 = jnp.bfloat16


def whole_layer(
    sps, tps, res, q, k, v, sinks, ow, gain, wgu, wd, out,
    kext, vext, att, abuf, mixed, nbuf, gubuf, dbuf, acc, hid, pbuf, cbuf, sbuf, r1, s1, r2, ssem, rsem,
):
    sp, tp = lax.axis_index("sp"), lax.axis_index("tp")
    g, p = sp // 2, sp % 2
    x, c = tp // 2, tp % 2
    groups = sps // 2
    rows, width = q.shape
    own, depth = res.shape
    cut = wd.shape[2]
    nblk = rows // WINDOW
    heads = width // HEAD
    slots = 2 * tps
    has_l, has_r = g > 0, g < groups - 1

    counter = [0]

    def fresh(n=1):
        counter[0] += n
        return counter[0] - n

    def copy(src, dst, ssem_at, rsem_at, to):
        return pltpu.make_async_remote_copy(
            src_ref=src, dst_ref=dst, send_sem=ssem.at[ssem_at], recv_sem=rsem.at[rsem_at],
            device_id=to, device_id_type=MESH,
        )

    sends = []

    def go(src, dst, rsem_at, to, cond=None):
        one = copy(src, dst, fresh(), rsem_at, to)
        sends.append((cond, one))
        if cond is None:
            one.start()
        else:
            pl.when(cond)(one.start)
        return one

    left, right = (jnp.maximum(sp - 2, 0), tp), (jnp.minimum(sp + 2, sps - 1), tp)
    ypeer = (g * 2 + 1 - p, tp)
    xpeer = (sp, (1 - x) * 2 + c)
    cpeer = (sp, x * 2 + 1 - c)
    dpeer = (sp, (1 - x) * 2 + 1 - c)
    halo_to = (jnp.minimum(sp + 1, sps - 1), tp)
    halo_from = (jnp.maximum(sp - 1, 0), tp)

    barrier = pltpu.get_barrier_semaphore()
    for peer in (ypeer, xpeer, cpeer, dpeer):
        pl.semaphore_signal(barrier, inc=1, device_id=peer, device_id_type=MESH)

    def greet(cond, peer):
        @pl.when(cond)
        def _():
            pl.semaphore_signal(barrier, inc=1, device_id=peer, device_id_type=MESH)

    greet(has_l, left)
    greet(has_r, right)
    greet(has_r & (p == 1), halo_to)
    greet(has_l & (p == 0), halo_from)
    one = lambda cond: jnp.where(cond, 1, 0)
    pl.semaphore_wait(
        barrier, 4 + one(has_l) + one(has_r) + one(has_r & (p == 1)) + one(has_l & (p == 0))
    )

    R_HK, R_HV, R_YG, R_YD = 0, 1, 2, 3
    R_GU = 4
    R_D = R_GU + 2 * groups
    R_A = R_D + 2 * groups
    R_N = R_A + 3
    R_C = R_N + slots
    R_1 = R_C + 2 * groups
    R_2 = R_1 + 2 * groups

    first = pl.ds(0, WINDOW)
    last = pl.ds(rows - WINDOW, WINDOW)
    halo_k = go(k.at[last], kext.at[first], R_HK, halo_to, sp < sps - 1)
    halo_v = go(v.at[last], vext.at[first], R_HV, halo_to, sp < sps - 1)
    go(wgu.at[1 - p], gubuf.at[g, p], R_YG, ypeer)
    go(wgu.at[p], gubuf.at[g, p], R_GU + 2 * g + p, right, has_r)
    go(wgu.at[p], gubuf.at[g, p], R_GU + 2 * g + p, left, has_l)
    go(wd.at[1 - p], dbuf.at[g, p], R_YD, ypeer)
    gubuf[g, p] = wgu[p]
    dbuf[g, p] = wd[p]

    def landed(buf, rsem_at):
        copy(buf, buf, 0, rsem_at, ypeer).wait_recv()

    kext[pl.ds(WINDOW, rows)] = k[...]
    vext[pl.ds(WINDOW, rows)] = v[...]

    @pl.when(sp == 0)
    def _():
        kext[first] = jnp.zeros((WINDOW, HEAD), BF16)
        vext[first] = jnp.zeros((WINDOW, HEAD), BF16)

    def attend_block(n):
        at = pl.multiple_of(n * WINDOW, WINDOW)
        qb = q[pl.ds(at, WINDOW), :]
        qs = jnp.concatenate([qb[:, h * HEAD : (h + 1) * HEAD] for h in range(heads)], axis=0)
        kb = kext[pl.ds(at, 2 * WINDOW), :]
        vb = vext[pl.ds(at, 2 * WINDOW), :]
        score = lax.dot_general(
            qs, kb, (((1,), (1,)), ((), ())), preferred_element_type=F32
        ) * HEAD ** (-0.5)
        rel = (
            lax.broadcasted_iota(jnp.int32, score.shape, 0) % WINDOW
            + WINDOW
            - lax.broadcasted_iota(jnp.int32, score.shape, 1)
        )
        col = lax.broadcasted_iota(jnp.int32, score.shape, 1)
        start = jnp.where(sp * nblk + n > 0, 0, WINDOW)
        score = jnp.where((rel >= 0) & (rel < WINDOW) & (col >= start), score, -jnp.inf)
        sink = jnp.concatenate(
            [jnp.full((WINDOW, 1), sinks[h], F32) for h in range(heads)], axis=0
        )
        top = jnp.maximum(jnp.max(score, axis=-1, keepdims=True), sink)
        expd = jnp.exp(score - top)
        denom = jnp.sum(expd, axis=-1, keepdims=True) + jnp.exp(sink - top)
        weights = (expd / denom).astype(BF16)
        res_ = jnp.dot(weights, vb, preferred_element_type=F32).astype(BF16)
        att[pl.ds(at, WINDOW), :] = jnp.concatenate(
            [res_[h * WINDOW : (h + 1) * WINDOW] for h in range(heads)], axis=1
        )

    pl.loop(1, nblk)(attend_block)
    pl.when(sp > 0)(halo_k.wait_recv)
    pl.when(sp > 0)(halo_v.wait_recv)
    attend_block(0)

    for i, (peer, who) in enumerate(((xpeer, xpeer[1]), (dpeer, dpeer[1]), (cpeer, cpeer[1]))):
        go(att.at[pl.ds(pl.multiple_of(who * own, own), own)], abuf.at[i], R_A + i, peer)

    landed(gubuf.at[g, 1 - p], R_YG)
    go(gubuf.at[g, 1 - p], gubuf.at[g, 1 - p], R_GU + 2 * g + 1 - p, right, has_r)
    go(gubuf.at[g, 1 - p], gubuf.at[g, 1 - p], R_GU + 2 * g + 1 - p, left, has_l)

    def ow_rows(who):
        return ow[pl.ds(pl.multiple_of(who * width, width), width), :]

    proj = jnp.dot(
        att[pl.ds(pl.multiple_of(tp * own, own), own), :], ow_rows(tp), preferred_element_type=F32
    )
    acc_p = acc.at[pl.ds(0, own)]
    for i, who in enumerate((xpeer[1], dpeer[1], cpeer[1])):
        landed(abuf.at[i], R_A + i)
        proj += jnp.dot(abuf[i], ow_rows(who), preferred_element_type=F32)
    mixed[...] = (res[...].astype(F32) + proj).astype(BF16)
    mixf = mixed[...].astype(F32)
    normed = (
        mixf * lax.rsqrt(jnp.mean(mixf * mixf, axis=-1, keepdims=True) + 1e-06) * gain[...]
    ).astype(BF16)

    def slot(pp, xx, cc):
        return (pp * 2 + xx) * 2 + cc

    def block(s, lo=0, n=None):
        return nbuf.at[pl.ds(pl.multiple_of(s * own, own), own), pl.ds(lo, n or depth)]

    mine = slot(p, x, c)
    nbuf[pl.ds(pl.multiple_of(mine * own, own), own), :] = normed
    half = depth // 2
    N_X, N_Y, N_DA, N_DB, N_C = R_N, R_N + 1, R_N + 2, R_N + 3, R_N + 4
    go(block(mine), block(mine), N_X, xpeer)
    go(block(mine), block(mine), N_Y, ypeer)
    go(block(mine), block(mine), N_C, cpeer)

    def order(n):
        near = jnp.minimum(g, groups - 1 - g)
        swing = g + (n // 2 if n % 2 == 0 else -((n + 1) // 2))
        far = jnp.where(g < groups - 1 - g, g + (n - near), g - (n - near))
        return jnp.where(n <= 2 * near, swing, far)

    def take(buf, base, n, jj):
        src = order(n)
        src = jnp.clip(src, 0, groups - 1)
        landed(buf.at[src, jj], base + 2 * src + jj)
        onward = ((src < g) & has_r) | ((src > g) & has_l)
        to = (jnp.where(src < g, right[0], left[0]), tp)
        go(buf.at[src, jj], buf.at[src, jj], base + 2 * src + jj, to, onward)

    take(gubuf, R_GU, 1, p)

    sx, sy, sd = slot(p, 1 - x, c), slot(1 - p, x, c), slot(1 - p, 1 - x, c)
    landed(block(sx), N_X)
    go(block(sx, 0, half), block(sx, 0, half), N_DA, ypeer)
    go(block(sx), block(sx), N_C + 1, cpeer)
    landed(block(sy), N_Y)
    go(block(sy, half, half), block(sy, half, half), N_DB, xpeer)
    go(block(sy), block(sy), N_C + 2, cpeer)
    take(gubuf, R_GU, 1, 1 - p)
    landed(block(sd, 0, half), N_DA)
    landed(block(sd, half, half), N_DB)
    go(block(sd), block(sd), N_C + 3, cpeer)
    landed(block(slot(p, x, 1 - c)), N_C)
    landed(block(slot(p, 1 - x, 1 - c)), N_C + 1)
    landed(block(slot(1 - p, x, 1 - c)), N_C + 2)
    landed(block(slot(1 - p, 1 - x, 1 - c)), N_C + 3)

    def add_block(src, jj, fresh_acc):
        at = pl.multiple_of((2 * src + jj) * cut, cut)

        @pl.loop(0, slots)
        def _(i):
            rs = pl.ds(pl.multiple_of(i * own, own), own)
            part = lax.dot_general(
                nbuf[rs, pl.ds(at, cut)], gubuf[src, jj],
                (((1,), (1,)), ((), ())), preferred_element_type=F32,
            )
            if fresh_acc:
                acc[rs, :] = part
            else:
                acc[rs, :] += part

    add_block(g, p, True)
    add_block(g, 1 - p, False)
    for n in range(1, groups):
        src = order(n)
        for i, jj in enumerate((p, 1 - p)):
            if n > 1:
                take(gubuf, R_GU, n, jj)
            add_block(src, jj, False)

    landed(dbuf.at[g, 1 - p], R_YD)
    for jj in (0, 1):
        go(dbuf.at[g, jj], dbuf.at[g, jj], R_D + 2 * g + jj, right, has_r)
        go(dbuf.at[g, jj], dbuf.at[g, jj], R_D + 2 * g + jj, left, has_l)

    ff = hid.shape[1]

    @pl.loop(0, slots)
    def _(i):
        rs = pl.ds(pl.multiple_of(i * own, own), own)
        both = acc[rs, :]
        gate, upper = both[:, :ff], both[:, ff:]
        hid[rs, :] = (jax.nn.silu(gate) * upper).astype(BF16)

    where = []

    def stage0(b):
        n, jj = b // 2, b % 2
        src = g if n == 0 else order(n)
        where.append(2 * src + jj)
        if n:
            take(dbuf, R_D, n, jj)

        @pl.loop(0, slots)
        def _(i):
            rs = pl.ds(pl.multiple_of(i * own, own), own)
            part = jnp.dot(hid[rs, :], dbuf[src, jj], preferred_element_type=F32)
            pbuf[b, i % 2, i // tps, (i // 2) % 2] = part.astype(BF16)

        go(pbuf.at[b, 1 - c], cbuf.at[b], R_C + b, cpeer)

    def stage1(b):
        landed(cbuf.at[b], R_C + b)
        sbuf[b] = (pbuf[b, c].astype(F32) + cbuf[b].astype(F32)).astype(BF16)
        if b % 2 == 0:
            go(sbuf.at[b, :, 1 - x], r1.at[b], R_1 + b, xpeer)
        else:
            go(sbuf.at[b, 1 - p], r1.at[b], R_1 + b, ypeer)

    def stage2(b):
        landed(r1.at[b], R_1 + b)
        kept = sbuf[b, :, x] if b % 2 == 0 else sbuf[b, p]
        s1[b] = (kept.astype(F32) + r1[b].astype(F32)).astype(BF16)
        if b % 2 == 0:
            go(s1.at[b, 1 - p], r2.at[b], R_2 + b, ypeer)
        else:
            go(s1.at[b, 1 - x], r2.at[b], R_2 + b, xpeer)

    def stage3(b):
        landed(r2.at[b], R_2 + b)
        kept = s1[b, p] if b % 2 == 0 else s1[b, x]
        cols = pl.ds(pl.multiple_of(where[b] * cut, cut), cut)
        out[:, cols] = (
            mixed[:, cols].astype(F32) + (kept.astype(F32) + r2[b].astype(F32))
        ).astype(BF16)

    stages = (stage0, stage1, stage2, stage3)
    total = 2 * groups
    for step in range(total + 3):
        for i, stage in enumerate(stages):
            if 0 <= step - i < total:
                stage(step - i)

    for cond, one_copy in sends:
        if cond is None:
            one_copy.wait_send()
        else:
            pl.when(cond)(one_copy.wait_send)


def layer(
    sps, tps, residual, queries, keys, values, sinks, out_weight, norm_gain,
    gate_weight, up_weight, down_weight,
):
    rows, width = queries.shape
    own, depth = residual.shape
    blk, ff = gate_weight.shape
    fits = (
        sps % 2 == 0 and 4 <= sps <= 8 and tps == 4 and keys.shape[1] == HEAD
        and blk % 128 == 0 and ff % 32 == 0 and own % 16 == 0
    )
    if not fits:
        return shards(
            residual, queries, keys, values, sinks, out_weight, norm_gain,
            gate_weight, up_weight, down_weight,
        )
    groups, ffh, slots = sps // 2, ff // 2, 2 * tps
    wgu = jnp.concatenate(
        [gate_weight.T.reshape(2, ffh, blk), up_weight.T.reshape(2, ffh, blk)], axis=1
    )
    wd = down_weight.reshape(2, ffh, blk)
    vm = pl.BlockSpec(memory_space=pltpu.VMEM)
    sm = pl.BlockSpec(memory_space=pltpu.SMEM)
    nb = 2 * groups
    return pl.pallas_call(
        functools.partial(whole_layer, sps, tps),
        out_shape=jax.ShapeDtypeStruct((own, depth), BF16),
        in_specs=[vm] * 4 + [sm] + [vm] * 4,
        out_specs=vm,
        scratch_shapes=[
            pltpu.VMEM((rows + WINDOW, HEAD), BF16),
            pltpu.VMEM((rows + WINDOW, HEAD), BF16),
            pltpu.VMEM((rows, width), BF16),
            pltpu.VMEM((3, own, width), BF16),
            pltpu.VMEM((own, depth), BF16),
            pltpu.VMEM((slots * own, depth), BF16),
            pltpu.VMEM((groups, 2, 2 * ffh, blk), BF16),
            pltpu.VMEM((groups, 2, ffh, blk), BF16),
            pltpu.VMEM((slots * own, 2 * ffh), F32),
            pltpu.VMEM((slots * own, ffh), BF16),
            pltpu.VMEM((nb, 2, 2, 2, own, blk), BF16),
            pltpu.VMEM((nb, 2, 2, own, blk), BF16),
            pltpu.VMEM((nb, 2, 2, own, blk), BF16),
            pltpu.VMEM((nb, 2, own, blk), BF16),
            pltpu.VMEM((nb, 2, own, blk), BF16),
            pltpu.VMEM((nb, own, blk), BF16),
            pltpu.SemaphoreType.DMA((24 * groups + 48,)),
            pltpu.SemaphoreType.DMA((24 * groups + 48,)),
        ],
        compiler_params=pltpu.CompilerParams(
            collective_id=0, has_side_effects=True, vmem_limit_bytes=66000000
        ),
        name="whole_layer",
    )(residual, queries, keys, values, sinks, out_weight, norm_gain.reshape(1, depth), wgu, wd)


def solution(mesh):
    placed = (
        P(("sp", "tp"), None),
        P("sp", "tp"),
        P("sp", "tp"),
        P("sp", "tp"),
        P("tp"),
        P(),
        P(),
        P("sp", "tp"),
        P("sp", "tp"),
        P("tp", "sp"),
    )
    return jax.shard_map(
        functools.partial(layer, mesh.shape["sp"], mesh.shape["tp"]), mesh=mesh, in_specs=placed, out_specs=P(("sp", "tp"), None), check_vma=False
    )
```

```python
import functools

import jax
import jax.numpy as jnp
from jax import lax
from jax.experimental import pallas as pl
from jax.experimental.pallas import tpu as pltpu
from jax.sharding import PartitionSpec as P

HEAD = 64
WINDOW = 128


def passed_along(block, axis, distance):
    devices = range(lax.axis_size(axis))
    route = [(i - distance, i) for i in devices if i - distance in devices]
    return lax.ppermute(block, axis, route)


def attend(queries, keys_ext, values_ext, sinks, block_base):
    rows = queries.shape[0]
    nblk = rows // WINDOW
    qheads = sinks.shape[0]
    kheads = keys_ext.shape[1] // HEAD
    group = qheads // kheads
    qblock = queries.reshape(nblk, WINDOW, kheads, group, HEAD).astype(jnp.float32)

    def band(arr):
        first = arr[:rows].reshape(nblk, WINDOW, kheads, HEAD)
        second = arr[WINDOW:].reshape(nblk, WINDOW, kheads, HEAD)
        return jnp.concatenate([first, second], axis=1).astype(jnp.float32)

    kband = band(keys_ext)
    vband = band(values_ext)
    score = jnp.einsum("nqhgd,nkhd->nhgqk", qblock, kband) * HEAD ** (-0.5)
    qidx = jnp.arange(WINDOW)[:, None]
    kidx = jnp.arange(2 * WINDOW)[None, :]
    rel = qidx + WINDOW - kidx
    valid = (rel >= 0) & (rel < WINDOW)
    blocks = block_base + jnp.arange(nblk)
    valid = valid[None] & ((blocks > 0)[:, None, None] | (kidx >= WINDOW)[None])
    score = jnp.where(valid[:, None, None], score, -jnp.inf)
    sink = sinks.reshape(kheads, group)[None, :, :, None]
    top = jnp.maximum(jnp.max(score, axis=-1), sink)
    expd = jnp.exp(score - top[..., None])
    denom = jnp.sum(expd, axis=-1) + jnp.exp(sink - top)
    weights = (expd / denom[..., None]).astype(jnp.bfloat16)
    result = jnp.einsum("nhgqk,nkhd->nqhgd", weights.astype(jnp.float32), vband)
    return result.reshape(rows, qheads * HEAD).astype(jnp.bfloat16)


def shards(
    residual,
    queries,
    keys,
    values,
    sinks,
    out_weight,
    norm_gain,
    gate_weight,
    up_weight,
    down_weight,
):
    rows_dev = queries.shape[0]
    prev_keys, prev_values = passed_along((keys[-WINDOW:], values[-WINDOW:]), "sp", 1)
    keys_ext = jnp.concatenate([prev_keys, keys], axis=0)
    values_ext = jnp.concatenate([prev_values, values], axis=0)
    attention = attend(
        queries, keys_ext, values_ext, sinks, lax.axis_index("sp") * (rows_dev // WINDOW)
    )
    width = attention.shape[1]
    mine = lax.dynamic_slice_in_dim(out_weight, lax.axis_index("tp") * width, width, 0)
    proj = lax.psum_scatter(
        jnp.dot(attention, mine, preferred_element_type=jnp.float32).astype(jnp.bfloat16),
        "tp",
        scatter_dimension=0,
        tiled=True,
    ).astype(jnp.float32)
    mixed = (residual.astype(jnp.float32) + proj).astype(jnp.bfloat16)
    mixf = mixed.astype(jnp.float32)
    normed = (
        mixf * lax.rsqrt(jnp.mean(mixf * mixf, axis=-1, keepdims=True) + 1e-06) * norm_gain
    ).astype(jnp.bfloat16)
    normed_all = lax.all_gather(normed, "tp", axis=0, tiled=True)
    gate = jnp.dot(
        normed_all,
        lax.all_gather(gate_weight, "sp", axis=0, tiled=True),
        preferred_element_type=jnp.float32,
    )
    upper = jnp.dot(
        normed_all,
        lax.all_gather(up_weight, "sp", axis=0, tiled=True),
        preferred_element_type=jnp.float32,
    )
    hidden = (jax.nn.silu(gate) * upper).astype(jnp.bfloat16)
    terms = jnp.dot(
        hidden,
        lax.all_gather(down_weight, "sp", axis=1, tiled=True),
        preferred_element_type=jnp.float32,
    )
    ffn = lax.psum_scatter(
        terms.astype(jnp.bfloat16), "tp", scatter_dimension=0, tiled=True
    ).astype(jnp.float32)
    return (mixed.astype(jnp.float32) + ffn).astype(jnp.bfloat16)


MESH = pl.DeviceIdType.MESH
F32 = jnp.float32
BF16 = jnp.bfloat16


def whole_layer(
    sps, tps, res, q, k, v, sinks, ow, gain, wgu, wd, out,
    kext, vext, att, abuf, mixed, nbuf, gubuf, dbuf, acc, hid, pbuf, cbuf, sbuf, r1, s1, r2, ssem, rsem,
):
    sp, tp = lax.axis_index("sp"), lax.axis_index("tp")
    g, p = sp // 2, sp % 2
    x, c = tp // 2, tp % 2
    groups = sps // 2
    rows, width = q.shape
    own, depth = res.shape
    cut = wd.shape[2]
    nblk = rows // WINDOW
    heads = width // HEAD
    slots = 2 * tps
    has_l, has_r = g > 0, g < groups - 1

    counter = [0]

    def fresh(n=1):
        counter[0] += n
        return counter[0] - n

    def copy(src, dst, ssem_at, rsem_at, to):
        return pltpu.make_async_remote_copy(
            src_ref=src, dst_ref=dst, send_sem=ssem.at[ssem_at], recv_sem=rsem.at[rsem_at],
            device_id=to, device_id_type=MESH,
        )

    sends = []

    def go(src, dst, rsem_at, to, cond=None):
        one = copy(src, dst, fresh(), rsem_at, to)
        sends.append((cond, one))
        if cond is None:
            one.start()
        else:
            pl.when(cond)(one.start)
        return one

    left, right = (jnp.maximum(sp - 2, 0), tp), (jnp.minimum(sp + 2, sps - 1), tp)
    ypeer = (g * 2 + 1 - p, tp)
    xpeer = (sp, (1 - x) * 2 + c)
    cpeer = (sp, x * 2 + 1 - c)
    dpeer = (sp, (1 - x) * 2 + 1 - c)
    halo_to = (jnp.minimum(sp + 1, sps - 1), tp)
    halo_from = (jnp.maximum(sp - 1, 0), tp)

    barrier = pltpu.get_barrier_semaphore()
    for peer in (ypeer, xpeer, cpeer, dpeer):
        pl.semaphore_signal(barrier, inc=1, device_id=peer, device_id_type=MESH)

    def greet(cond, peer):
        @pl.when(cond)
        def _():
            pl.semaphore_signal(barrier, inc=1, device_id=peer, device_id_type=MESH)

    greet(has_l, left)
    greet(has_r, right)
    greet(has_r & (p == 1), halo_to)
    greet(has_l & (p == 0), halo_from)
    one = lambda cond: jnp.where(cond, 1, 0)
    pl.semaphore_wait(
        barrier, 4 + one(has_l) + one(has_r) + one(has_r & (p == 1)) + one(has_l & (p == 0))
    )

    R_HK, R_HV, R_YG, R_YD = 0, 1, 2, 3
    R_GU = 4
    R_D = R_GU + 2 * groups
    R_A = R_D + 2 * groups
    R_N = R_A + 3
    R_C = R_N + slots
    R_1 = R_C + 2 * groups
    R_2 = R_1 + 2 * groups

    first = pl.ds(0, WINDOW)
    last = pl.ds(rows - WINDOW, WINDOW)
    halo_k = go(k.at[last], kext.at[first], R_HK, halo_to, sp < sps - 1)
    halo_v = go(v.at[last], vext.at[first], R_HV, halo_to, sp < sps - 1)
    go(wgu.at[1 - p], gubuf.at[g, p], R_YG, ypeer)
    go(wgu.at[p], gubuf.at[g, p], R_GU + 2 * g + p, right, has_r)
    go(wgu.at[p], gubuf.at[g, p], R_GU + 2 * g + p, left, has_l)
    go(wd.at[1 - p], dbuf.at[g, p], R_YD, ypeer)
    for side, cond in ((right, has_r), (left, has_l)):
        go(wd.at[p], dbuf.at[g, p], R_D + 2 * g + p, side, cond)
    gubuf[g, p] = wgu[p]
    dbuf[g, p] = wd[p]

    def landed(buf, rsem_at):
        copy(buf, buf, 0, rsem_at, ypeer).wait_recv()

    kext[pl.ds(WINDOW, rows)] = k[...]
    vext[pl.ds(WINDOW, rows)] = v[...]

    @pl.when(sp == 0)
    def _():
        kext[first] = jnp.zeros((WINDOW, HEAD), BF16)
        vext[first] = jnp.zeros((WINDOW, HEAD), BF16)

    def attend_block(n):
        at = pl.multiple_of(n * WINDOW, WINDOW)
        qb = q[pl.ds(at, WINDOW), :]
        qs = jnp.concatenate([qb[:, h * HEAD : (h + 1) * HEAD] for h in range(heads)], axis=0)
        kb = kext[pl.ds(at, 2 * WINDOW), :]
        vb = vext[pl.ds(at, 2 * WINDOW), :]
        score = lax.dot_general(
            qs, kb, (((1,), (1,)), ((), ())), preferred_element_type=F32
        ) * HEAD ** (-0.5)
        rel = (
            lax.broadcasted_iota(jnp.int32, score.shape, 0) % WINDOW
            + WINDOW
            - lax.broadcasted_iota(jnp.int32, score.shape, 1)
        )
        col = lax.broadcasted_iota(jnp.int32, score.shape, 1)
        start = jnp.where(sp * nblk + n > 0, 0, WINDOW)
        score = jnp.where((rel >= 0) & (rel < WINDOW) & (col >= start), score, -jnp.inf)
        sink = jnp.concatenate(
            [jnp.full((WINDOW, 1), sinks[h], F32) for h in range(heads)], axis=0
        )
        top = jnp.maximum(jnp.max(score, axis=-1, keepdims=True), sink)
        expd = jnp.exp(score - top)
        denom = jnp.sum(expd, axis=-1, keepdims=True) + jnp.exp(sink - top)
        weights = (expd / denom).astype(BF16)
        res_ = jnp.dot(weights, vb, preferred_element_type=F32).astype(BF16)
        att[pl.ds(at, WINDOW), :] = jnp.concatenate(
            [res_[h * WINDOW : (h + 1) * WINDOW] for h in range(heads)], axis=1
        )

    pl.loop(1, nblk // 2)(attend_block)

    landed(gubuf.at[g, 1 - p], R_YG)
    for side, cond in ((right, has_r), (left, has_l)):
        go(gubuf.at[g, 1 - p], gubuf.at[g, 1 - p], R_GU + 2 * g + 1 - p, side, cond)
    pl.loop(nblk // 2, nblk)(attend_block)
    pl.when(sp > 0)(halo_k.wait_recv)
    pl.when(sp > 0)(halo_v.wait_recv)
    attend_block(0)

    for i, (peer, who) in enumerate(((xpeer, xpeer[1]), (dpeer, dpeer[1]), (cpeer, cpeer[1]))):
        go(att.at[pl.ds(pl.multiple_of(who * own, own), own)], abuf.at[i], R_A + i, peer)

    landed(dbuf.at[g, 1 - p], R_YD)
    for side, cond in ((right, has_r), (left, has_l)):
        go(dbuf.at[g, 1 - p], dbuf.at[g, 1 - p], R_D + 2 * g + 1 - p, side, cond)

    def ow_rows(who):
        return ow[pl.ds(pl.multiple_of(who * width, width), width), :]

    proj = jnp.dot(
        att[pl.ds(pl.multiple_of(tp * own, own), own), :], ow_rows(tp), preferred_element_type=F32
    )
    acc_p = acc.at[pl.ds(0, own)]
    for i, who in enumerate((xpeer[1], dpeer[1], cpeer[1])):
        landed(abuf.at[i], R_A + i)
        proj += jnp.dot(abuf[i], ow_rows(who), preferred_element_type=F32)
    mixed[...] = (res[...].astype(F32) + proj).astype(BF16)
    mixf = mixed[...].astype(F32)
    normed = (
        mixf * lax.rsqrt(jnp.mean(mixf * mixf, axis=-1, keepdims=True) + 1e-06) * gain[...]
    ).astype(BF16)

    def slot(pp, xx, cc):
        return (pp * 2 + xx) * 2 + cc

    def block(s, lo=0, n=None):
        return nbuf.at[pl.ds(pl.multiple_of(s * own, own), own), pl.ds(lo, n or depth)]

    mine = slot(p, x, c)
    nbuf[pl.ds(pl.multiple_of(mine * own, own), own), :] = normed
    half = depth // 2
    N_X, N_Y, N_DA, N_DB, N_C = R_N, R_N + 1, R_N + 2, R_N + 3, R_N + 4
    go(block(mine), block(mine), N_X, xpeer)
    go(block(mine), block(mine), N_Y, ypeer)
    go(block(mine), block(mine), N_C, cpeer)

    def order(n):
        near = jnp.minimum(g, groups - 1 - g)
        swing = g + (n // 2 if n % 2 == 0 else -((n + 1) // 2))
        far = jnp.where(g < groups - 1 - g, g + (n - near), g - (n - near))
        return jnp.where(n <= 2 * near, swing, far)

    other = 1 - p
    arrivals = {}
    for base, buf in ((R_GU, gubuf), (R_D, dbuf)):
        for n in range(1, groups):
            src = jnp.clip(order(n), 0, groups - 1)
            onward = ((src < g) & has_r) | ((src > g) & has_l)
            to = (jnp.where(src < g, right[0], left[0]), tp)
            for jj in (p, other):
                ref, at = buf.at[src, jj], base + 2 * src + jj
                hop = copy(ref, ref, fresh(), at, to)
                sends.append((onward, hop))
                arrivals[base, n, jj is p] = (onward, copy(ref, ref, 0, at, ypeer), hop)

    def take(base, n, jj, cond=None):
        onward, arrived, hop = arrivals[base, n, jj is p]
        if cond is None:
            arrived.wait_recv()
            pl.when(onward)(hop.start)
        else:
            pl.when(cond)(arrived.wait_recv)
            pl.when(cond & onward)(hop.start)

    near = jnp.minimum(g, groups - 1 - g)
    early = groups - 2

    def take_early(base, jj):
        take(base, 1, jj)
        for n in range(2, early + 1):
            take(base, n, jj, n <= 2 * near)

    def take_late(base, n, jj):
        if n > early:
            take(base, n, jj)
        elif n > 1:
            take(base, n, jj, n > 2 * near)

    sx, sy, sd = slot(p, 1 - x, c), slot(1 - p, x, c), slot(1 - p, 1 - x, c)
    take_early(R_GU, p)
    landed(block(sx), N_X)
    go(block(sx, 0, half), block(sx, 0, half), N_DA, ypeer)
    go(block(sx), block(sx), N_C + 1, cpeer)
    landed(block(sy), N_Y)
    go(block(sy, half, half), block(sy, half, half), N_DB, xpeer)
    go(block(sy), block(sy), N_C + 2, cpeer)
    take_early(R_GU, other)
    landed(block(sd, 0, half), N_DA)
    landed(block(sd, half, half), N_DB)
    go(block(sd), block(sd), N_C + 3, cpeer)
    landed(block(slot(p, x, 1 - c)), N_C)
    landed(block(slot(p, 1 - x, 1 - c)), N_C + 1)
    landed(block(slot(1 - p, x, 1 - c)), N_C + 2)
    landed(block(slot(1 - p, 1 - x, 1 - c)), N_C + 3)

    def add_block(src, jj, fresh_acc):
        at = pl.multiple_of((2 * src + jj) * cut, cut)

        @pl.loop(0, slots)
        def _(i):
            rs = pl.ds(pl.multiple_of(i * own, own), own)
            part = lax.dot_general(
                nbuf[rs, pl.ds(at, cut)], gubuf[src, jj],
                (((1,), (1,)), ((), ())), preferred_element_type=F32,
            )
            if fresh_acc:
                acc[rs, :] = part
            else:
                acc[rs, :] += part

    add_block(g, p, True)
    add_block(g, 1 - p, False)
    for n in range(1, groups):
        src = order(n)
        for jj in (p, other):
            take_late(R_GU, n, jj)
            if n == groups - 1 and jj is other:
                for dj in (p, other):
                    take_early(R_D, dj)
            add_block(src, jj, False)

    ff = hid.shape[1]

    @pl.loop(0, slots)
    def _(i):
        rs = pl.ds(pl.multiple_of(i * own, own), own)
        both = acc[rs, :]
        gate, upper = both[:, :ff], both[:, ff:]
        hid[rs, :] = (jax.nn.silu(gate) * upper).astype(BF16)

    where = []

    def stage0(b):
        n, jj = b // 2, b % 2
        src = g if n == 0 else order(n)
        where.append(2 * src + jj)
        if n > 1 and jj == 0:
            for dj in (p, other):
                take_late(R_D, n, dj)

        @pl.loop(0, slots)
        def _(i):
            rs = pl.ds(pl.multiple_of(i * own, own), own)
            part = jnp.dot(hid[rs, :], dbuf[src, jj], preferred_element_type=F32)
            pbuf[b, i % 2, i // tps, (i // 2) % 2] = part.astype(BF16)

        go(pbuf.at[b, 1 - c], cbuf.at[b], R_C + b, cpeer)

    def stage1(b):
        landed(cbuf.at[b], R_C + b)
        sbuf[b] = (pbuf[b, c].astype(F32) + cbuf[b].astype(F32)).astype(BF16)
        if b % 2 == 0:
            go(sbuf.at[b, :, 1 - x], r1.at[b], R_1 + b, xpeer)
        else:
            go(sbuf.at[b, 1 - p], r1.at[b], R_1 + b, ypeer)

    def stage2(b):
        landed(r1.at[b], R_1 + b)
        kept = sbuf[b, :, x] if b % 2 == 0 else sbuf[b, p]
        s1[b] = (kept.astype(F32) + r1[b].astype(F32)).astype(BF16)
        if b % 2 == 0:
            go(s1.at[b, 1 - p], r2.at[b], R_2 + b, ypeer)
        else:
            go(s1.at[b, 1 - x], r2.at[b], R_2 + b, xpeer)

    def stage3(b):
        landed(r2.at[b], R_2 + b)
        kept = s1[b, p] if b % 2 == 0 else s1[b, x]
        cols = pl.ds(pl.multiple_of(where[b] * cut, cut), cut)
        out[:, cols] = (
            mixed[:, cols].astype(F32) + (kept.astype(F32) + r2[b].astype(F32))
        ).astype(BF16)

    stages = (stage0, stage1, stage2, stage3)
    total = 2 * groups
    for step in range(total + 3):
        for i, stage in enumerate(stages):
            if 0 <= step - i < total:
                stage(step - i)

    for cond, one_copy in sends:
        if cond is None:
            one_copy.wait_send()
        else:
            pl.when(cond)(one_copy.wait_send)


def layer(
    sps, tps, residual, queries, keys, values, sinks, out_weight, norm_gain,
    gate_weight, up_weight, down_weight,
):
    rows, width = queries.shape
    own, depth = residual.shape
    blk, ff = gate_weight.shape
    fits = (
        sps % 2 == 0 and 4 <= sps <= 8 and tps == 4 and keys.shape[1] == HEAD
        and blk % 128 == 0 and ff % 32 == 0 and own % 16 == 0
    )
    if not fits:
        return shards(
            residual, queries, keys, values, sinks, out_weight, norm_gain,
            gate_weight, up_weight, down_weight,
        )
    groups, ffh, slots = sps // 2, ff // 2, 2 * tps
    wgu = jnp.concatenate(
        [gate_weight.T.reshape(2, ffh, blk), up_weight.T.reshape(2, ffh, blk)], axis=1
    )
    wd = down_weight.reshape(2, ffh, blk)
    vm = pl.BlockSpec(memory_space=pltpu.VMEM)
    sm = pl.BlockSpec(memory_space=pltpu.SMEM)
    nb = 2 * groups
    return pl.pallas_call(
        functools.partial(whole_layer, sps, tps),
        out_shape=jax.ShapeDtypeStruct((own, depth), BF16),
        in_specs=[vm] * 4 + [sm] + [vm] * 4,
        out_specs=vm,
        scratch_shapes=[
            pltpu.VMEM((rows + WINDOW, HEAD), BF16),
            pltpu.VMEM((rows + WINDOW, HEAD), BF16),
            pltpu.VMEM((rows, width), BF16),
            pltpu.VMEM((3, own, width), BF16),
            pltpu.VMEM((own, depth), BF16),
            pltpu.VMEM((slots * own, depth), BF16),
            pltpu.VMEM((groups, 2, 2 * ffh, blk), BF16),
            pltpu.VMEM((groups, 2, ffh, blk), BF16),
            pltpu.VMEM((slots * own, 2 * ffh), F32),
            pltpu.VMEM((slots * own, ffh), BF16),
            pltpu.VMEM((nb, 2, 2, 2, own, blk), BF16),
            pltpu.VMEM((nb, 2, 2, own, blk), BF16),
            pltpu.VMEM((nb, 2, 2, own, blk), BF16),
            pltpu.VMEM((nb, 2, own, blk), BF16),
            pltpu.VMEM((nb, 2, own, blk), BF16),
            pltpu.VMEM((nb, own, blk), BF16),
            pltpu.SemaphoreType.DMA((24 * groups + 48,)),
            pltpu.SemaphoreType.DMA((24 * groups + 48,)),
        ],
        compiler_params=pltpu.CompilerParams(
            collective_id=0, has_side_effects=True, vmem_limit_bytes=66000000
        ),
        name="whole_layer",
    )(residual, queries, keys, values, sinks, out_weight, norm_gain.reshape(1, depth), wgu, wd)


def solution(mesh):
    placed = (
        P(("sp", "tp"), None),
        P("sp", "tp"),
        P("sp", "tp"),
        P("sp", "tp"),
        P("tp"),
        P(),
        P(),
        P("sp", "tp"),
        P("sp", "tp"),
        P("tp", "sp"),
    )
    return jax.shard_map(
        functools.partial(layer, mesh.shape["sp"], mesh.shape["tp"]), mesh=mesh, in_specs=placed, out_specs=P(("sp", "tp"), None), check_vma=False
    )
```

```python
import functools

import jax
import jax.numpy as jnp
from jax import lax
from jax.experimental import pallas as pl
from jax.experimental.pallas import tpu as pltpu
from jax.sharding import PartitionSpec as P

HEAD = 64
WINDOW = 128


def passed_along(block, axis, distance):
    devices = range(lax.axis_size(axis))
    route = [(i - distance, i) for i in devices if i - distance in devices]
    return lax.ppermute(block, axis, route)


def attend(queries, keys_ext, values_ext, sinks, block_base):
    rows = queries.shape[0]
    nblk = rows // WINDOW
    qheads = sinks.shape[0]
    kheads = keys_ext.shape[1] // HEAD
    group = qheads // kheads
    qblock = queries.reshape(nblk, WINDOW, kheads, group, HEAD).astype(jnp.float32)

    def band(arr):
        first = arr[:rows].reshape(nblk, WINDOW, kheads, HEAD)
        second = arr[WINDOW:].reshape(nblk, WINDOW, kheads, HEAD)
        return jnp.concatenate([first, second], axis=1).astype(jnp.float32)

    kband = band(keys_ext)
    vband = band(values_ext)
    score = jnp.einsum("nqhgd,nkhd->nhgqk", qblock, kband) * HEAD ** (-0.5)
    qidx = jnp.arange(WINDOW)[:, None]
    kidx = jnp.arange(2 * WINDOW)[None, :]
    rel = qidx + WINDOW - kidx
    valid = (rel >= 0) & (rel < WINDOW)
    blocks = block_base + jnp.arange(nblk)
    valid = valid[None] & ((blocks > 0)[:, None, None] | (kidx >= WINDOW)[None])
    score = jnp.where(valid[:, None, None], score, -jnp.inf)
    sink = sinks.reshape(kheads, group)[None, :, :, None]
    top = jnp.maximum(jnp.max(score, axis=-1), sink)
    expd = jnp.exp(score - top[..., None])
    denom = jnp.sum(expd, axis=-1) + jnp.exp(sink - top)
    weights = (expd / denom[..., None]).astype(jnp.bfloat16)
    result = jnp.einsum("nhgqk,nkhd->nqhgd", weights.astype(jnp.float32), vband)
    return result.reshape(rows, qheads * HEAD).astype(jnp.bfloat16)


def shards(
    residual,
    queries,
    keys,
    values,
    sinks,
    out_weight,
    norm_gain,
    gate_weight,
    up_weight,
    down_weight,
):
    rows_dev = queries.shape[0]
    prev_keys, prev_values = passed_along((keys[-WINDOW:], values[-WINDOW:]), "sp", 1)
    keys_ext = jnp.concatenate([prev_keys, keys], axis=0)
    values_ext = jnp.concatenate([prev_values, values], axis=0)
    attention = attend(
        queries, keys_ext, values_ext, sinks, lax.axis_index("sp") * (rows_dev // WINDOW)
    )
    width = attention.shape[1]
    mine = lax.dynamic_slice_in_dim(out_weight, lax.axis_index("tp") * width, width, 0)
    proj = lax.psum_scatter(
        jnp.dot(attention, mine, preferred_element_type=jnp.float32).astype(jnp.bfloat16),
        "tp",
        scatter_dimension=0,
        tiled=True,
    ).astype(jnp.float32)
    mixed = (residual.astype(jnp.float32) + proj).astype(jnp.bfloat16)
    mixf = mixed.astype(jnp.float32)
    normed = (
        mixf * lax.rsqrt(jnp.mean(mixf * mixf, axis=-1, keepdims=True) + 1e-06) * norm_gain
    ).astype(jnp.bfloat16)
    normed_all = lax.all_gather(normed, "tp", axis=0, tiled=True)
    gate = jnp.dot(
        normed_all,
        lax.all_gather(gate_weight, "sp", axis=0, tiled=True),
        preferred_element_type=jnp.float32,
    )
    upper = jnp.dot(
        normed_all,
        lax.all_gather(up_weight, "sp", axis=0, tiled=True),
        preferred_element_type=jnp.float32,
    )
    hidden = (jax.nn.silu(gate) * upper).astype(jnp.bfloat16)
    terms = jnp.dot(
        hidden,
        lax.all_gather(down_weight, "sp", axis=1, tiled=True),
        preferred_element_type=jnp.float32,
    )
    ffn = lax.psum_scatter(
        terms.astype(jnp.bfloat16), "tp", scatter_dimension=0, tiled=True
    ).astype(jnp.float32)
    return (mixed.astype(jnp.float32) + ffn).astype(jnp.bfloat16)


MESH = pl.DeviceIdType.MESH
F32 = jnp.float32
BF16 = jnp.bfloat16


def whole_layer(
    sps, tps, res, q, k, v, sinks, ow_hbm, gain, wgu, wd, out,
    kext, vext, att, abuf, mixed, nbuf, gubuf, dbuf, acc, hid, pbuf, cbuf, sbuf, r1, s1, r2, ow, osem, ssem, rsem,
):
    sp, tp = lax.axis_index("sp"), lax.axis_index("tp")
    g, p = sp // 2, sp % 2
    x, c = tp // 2, tp % 2
    groups = sps // 2
    rows, width = q.shape
    own, depth = res.shape
    cut = wd.shape[2]
    nblk = rows // WINDOW
    heads = width // HEAD
    slots = 2 * tps
    has_l, has_r = g > 0, g < groups - 1

    counter = [0]

    def fresh(n=1):
        counter[0] += n
        return counter[0] - n

    def copy(src, dst, ssem_at, rsem_at, to):
        return pltpu.make_async_remote_copy(
            src_ref=src, dst_ref=dst, send_sem=ssem.at[ssem_at], recv_sem=rsem.at[rsem_at],
            device_id=to, device_id_type=MESH,
        )

    sends = []

    def go(src, dst, rsem_at, to, cond=None):
        one = copy(src, dst, fresh(), rsem_at, to)
        sends.append((cond, one))
        if cond is None:
            one.start()
        else:
            pl.when(cond)(one.start)
        return one

    left, right = (jnp.maximum(sp - 2, 0), tp), (jnp.minimum(sp + 2, sps - 1), tp)
    ypeer = (g * 2 + 1 - p, tp)
    xpeer = (sp, (1 - x) * 2 + c)
    cpeer = (sp, x * 2 + 1 - c)
    dpeer = (sp, (1 - x) * 2 + 1 - c)
    halo_to = (jnp.minimum(sp + 1, sps - 1), tp)
    halo_from = (jnp.maximum(sp - 1, 0), tp)

    barrier = pltpu.get_barrier_semaphore()
    for peer in (ypeer, xpeer, cpeer, dpeer):
        pl.semaphore_signal(barrier, inc=1, device_id=peer, device_id_type=MESH)

    def greet(cond, peer):
        @pl.when(cond)
        def _():
            pl.semaphore_signal(barrier, inc=1, device_id=peer, device_id_type=MESH)

    greet(has_l, left)
    greet(has_r, right)
    greet(has_r & (p == 1), halo_to)
    greet(has_l & (p == 0), halo_from)
    one = lambda cond: jnp.where(cond, 1, 0)
    pl.semaphore_wait(
        barrier, 4 + one(has_l) + one(has_r) + one(has_r & (p == 1)) + one(has_l & (p == 0))
    )

    R_HK, R_HV, R_YG, R_YD = 0, 1, 2, 3
    R_GU = 4
    R_D = R_GU + 2 * groups
    R_A = R_D + 2 * groups
    R_N = R_A + 3
    R_C = R_N + slots
    R_1 = R_C + 2 * groups
    R_2 = R_1 + 2 * groups

    first = pl.ds(0, WINDOW)
    last = pl.ds(rows - WINDOW, WINDOW)
    halo_k = go(k.at[last], kext.at[first], R_HK, halo_to, sp < sps - 1)
    halo_v = go(v.at[last], vext.at[first], R_HV, halo_to, sp < sps - 1)
    go(wgu.at[1 - p], gubuf.at[g, p], R_YG, ypeer)
    go(wgu.at[p], gubuf.at[g, p], R_GU + 2 * g + p, right, has_r)
    go(wgu.at[p], gubuf.at[g, p], R_GU + 2 * g + p, left, has_l)
    go(wd.at[1 - p], dbuf.at[g, p], R_YD, ypeer)
    for side, cond in ((right, has_r), (left, has_l)):
        go(wd.at[p], dbuf.at[g, p], R_D + 2 * g + p, side, cond)
    fetch = pltpu.make_async_copy(ow_hbm, ow, osem)
    fetch.start()
    gubuf[g, p] = wgu[p]
    dbuf[g, p] = wd[p]

    def landed(buf, rsem_at):
        copy(buf, buf, 0, rsem_at, ypeer).wait_recv()

    kext[pl.ds(WINDOW, rows)] = k[...]
    vext[pl.ds(WINDOW, rows)] = v[...]

    @pl.when(sp == 0)
    def _():
        kext[first] = jnp.zeros((WINDOW, HEAD), BF16)
        vext[first] = jnp.zeros((WINDOW, HEAD), BF16)

    def attend_block(n):
        at = pl.multiple_of(n * WINDOW, WINDOW)
        qb = q[pl.ds(at, WINDOW), :]
        qs = jnp.concatenate([qb[:, h * HEAD : (h + 1) * HEAD] for h in range(heads)], axis=0)
        kb = kext[pl.ds(at, 2 * WINDOW), :]
        vb = vext[pl.ds(at, 2 * WINDOW), :]
        score = lax.dot_general(
            qs, kb, (((1,), (1,)), ((), ())), preferred_element_type=F32
        ) * HEAD ** (-0.5)
        rel = (
            lax.broadcasted_iota(jnp.int32, score.shape, 0) % WINDOW
            + WINDOW
            - lax.broadcasted_iota(jnp.int32, score.shape, 1)
        )
        col = lax.broadcasted_iota(jnp.int32, score.shape, 1)
        start = jnp.where(sp * nblk + n > 0, 0, WINDOW)
        score = jnp.where((rel >= 0) & (rel < WINDOW) & (col >= start), score, -jnp.inf)
        sink = jnp.concatenate(
            [jnp.full((WINDOW, 1), sinks[h], F32) for h in range(heads)], axis=0
        )
        top = jnp.maximum(jnp.max(score, axis=-1, keepdims=True), sink)
        expd = jnp.exp(score - top)
        denom = jnp.sum(expd, axis=-1, keepdims=True) + jnp.exp(sink - top)
        weights = (expd / denom).astype(BF16)
        res_ = jnp.dot(weights, vb, preferred_element_type=F32).astype(BF16)
        att[pl.ds(at, WINDOW), :] = jnp.concatenate(
            [res_[h * WINDOW : (h + 1) * WINDOW] for h in range(heads)], axis=1
        )

    pl.loop(1, nblk // 2)(attend_block)

    landed(gubuf.at[g, 1 - p], R_YG)
    for side, cond in ((right, has_r), (left, has_l)):
        go(gubuf.at[g, 1 - p], gubuf.at[g, 1 - p], R_GU + 2 * g + 1 - p, side, cond)
    pl.loop(nblk // 2, nblk)(attend_block)
    pl.when(sp > 0)(halo_k.wait_recv)
    pl.when(sp > 0)(halo_v.wait_recv)
    attend_block(0)

    for i, (peer, who) in enumerate(((xpeer, xpeer[1]), (dpeer, dpeer[1]), (cpeer, cpeer[1]))):
        go(att.at[pl.ds(pl.multiple_of(who * own, own), own)], abuf.at[i], R_A + i, peer)

    landed(dbuf.at[g, 1 - p], R_YD)
    for side, cond in ((right, has_r), (left, has_l)):
        go(dbuf.at[g, 1 - p], dbuf.at[g, 1 - p], R_D + 2 * g + 1 - p, side, cond)

    def ow_rows(who):
        return ow[pl.ds(pl.multiple_of(who * width, width), width), :]

    fetch.wait()
    proj = jnp.dot(
        att[pl.ds(pl.multiple_of(tp * own, own), own), :], ow_rows(tp), preferred_element_type=F32
    )
    acc_p = acc.at[pl.ds(0, own)]
    for i, who in enumerate((xpeer[1], dpeer[1], cpeer[1])):
        landed(abuf.at[i], R_A + i)
        proj += jnp.dot(abuf[i], ow_rows(who), preferred_element_type=F32)
    mixed[...] = (res[...].astype(F32) + proj).astype(BF16)
    mixf = mixed[...].astype(F32)
    normed = (
        mixf * lax.rsqrt(jnp.mean(mixf * mixf, axis=-1, keepdims=True) + 1e-06) * gain[...]
    ).astype(BF16)

    def slot(pp, xx, cc):
        return (pp * 2 + xx) * 2 + cc

    def block(s, lo=0, n=None):
        return nbuf.at[pl.ds(pl.multiple_of(s * own, own), own), pl.ds(lo, n or depth)]

    mine = slot(p, x, c)
    nbuf[pl.ds(pl.multiple_of(mine * own, own), own), :] = normed
    half = depth // 2
    N_X, N_Y, N_DA, N_DB, N_C = R_N, R_N + 1, R_N + 2, R_N + 3, R_N + 4
    go(block(mine), block(mine), N_X, xpeer)
    go(block(mine), block(mine), N_Y, ypeer)
    go(block(mine), block(mine), N_C, cpeer)

    def order(n):
        near = jnp.minimum(g, groups - 1 - g)
        swing = g + (n // 2 if n % 2 == 0 else -((n + 1) // 2))
        far = jnp.where(g < groups - 1 - g, g + (n - near), g - (n - near))
        return jnp.where(n <= 2 * near, swing, far)

    other = 1 - p
    arrivals = {}
    key = lambda jj: jj if isinstance(jj, int) else jj is p
    for base, buf in ((R_GU, gubuf), (R_D, dbuf)):
        for n in range(1, groups):
            src = jnp.clip(order(n), 0, groups - 1)
            onward = ((src < g) & has_r) | ((src > g) & has_l)
            to = (jnp.where(src < g, right[0], left[0]), tp)
            for jj in (p, other) if base == R_GU else (0, 1):
                ref, at = buf.at[src, jj], base + 2 * src + jj
                hop = copy(ref, ref, fresh(), at, to)
                sends.append((onward, hop))
                arrivals[base, n, key(jj)] = (onward, copy(ref, ref, 0, at, ypeer), hop)

    def take(base, n, jj, cond=None):
        onward, arrived, hop = arrivals[base, n, key(jj)]
        if cond is None:
            arrived.wait_recv()
            pl.when(onward)(hop.start)
        else:
            pl.when(cond)(arrived.wait_recv)
            pl.when(cond & onward)(hop.start)

    near = jnp.minimum(g, groups - 1 - g)
    early = groups - 2

    def take_early(base, jj):
        take(base, 1, jj)
        for n in range(2, early + 1):
            take(base, n, jj, n <= 2 * near)

    def take_late(base, n, jj):
        if n > early:
            take(base, n, jj)
        elif n > 1:
            take(base, n, jj, n > 2 * near)

    sx, sy, sd = slot(p, 1 - x, c), slot(1 - p, x, c), slot(1 - p, 1 - x, c)
    take_early(R_GU, p)
    landed(block(sx), N_X)
    go(block(sx, 0, half), block(sx, 0, half), N_DA, ypeer)
    go(block(sx), block(sx), N_C + 1, cpeer)
    landed(block(sy), N_Y)
    go(block(sy, half, half), block(sy, half, half), N_DB, xpeer)
    go(block(sy), block(sy), N_C + 2, cpeer)
    take_early(R_GU, other)
    landed(block(sd, 0, half), N_DA)
    landed(block(sd, half, half), N_DB)
    go(block(sd), block(sd), N_C + 3, cpeer)
    landed(block(slot(p, x, 1 - c)), N_C)
    landed(block(slot(p, 1 - x, 1 - c)), N_C + 1)
    landed(block(slot(1 - p, x, 1 - c)), N_C + 2)
    landed(block(slot(1 - p, 1 - x, 1 - c)), N_C + 3)

    def add_block(src, jj, fresh_acc):
        at = pl.multiple_of((2 * src + jj) * cut, cut)

        @pl.loop(0, slots)
        def _(i):
            rs = pl.ds(pl.multiple_of(i * own, own), own)
            part = lax.dot_general(
                nbuf[rs, pl.ds(at, cut)], gubuf[src, jj],
                (((1,), (1,)), ((), ())), preferred_element_type=F32,
            )
            if fresh_acc:
                acc[rs, :] = part
            else:
                acc[rs, :] += part

    add_block(g, p, True)
    add_block(g, 1 - p, False)
    for n in range(1, groups):
        src = order(n)
        for jj in (p, other):
            take_late(R_GU, n, jj)
            if n == groups - 1 and jj is other:
                for dj in (0, 1):
                    take_early(R_D, dj)
            add_block(src, jj, False)

    ff = hid.shape[1]

    @pl.loop(0, slots)
    def _(i):
        rs = pl.ds(pl.multiple_of(i * own, own), own)
        both = acc[rs, :]
        gate, upper = both[:, :ff], both[:, ff:]
        hid[rs, :] = (jax.nn.silu(gate) * upper).astype(BF16)

    where = []

    def stage0(b):
        n, jj = b // 2, b % 2
        src = g if n == 0 else order(n)
        where.append(2 * src + jj)
        if n > 1:
            take_late(R_D, n, jj)

        @pl.loop(0, slots)
        def _(i):
            rs = pl.ds(pl.multiple_of(i * own, own), own)
            part = jnp.dot(hid[rs, :], dbuf[src, jj], preferred_element_type=F32)
            pbuf[b, i % 2, i // tps, (i // 2) % 2] = part.astype(BF16)

        go(pbuf.at[b, 1 - c], cbuf.at[b], R_C + b, cpeer)

    def stage1(b):
        landed(cbuf.at[b], R_C + b)
        sbuf[b] = (pbuf[b, c].astype(F32) + cbuf[b].astype(F32)).astype(BF16)
        if b % 2 == 0:
            go(sbuf.at[b, :, 1 - x], r1.at[b], R_1 + b, xpeer)
        else:
            go(sbuf.at[b, 1 - p], r1.at[b], R_1 + b, ypeer)

    def stage2(b):
        landed(r1.at[b], R_1 + b)
        kept = sbuf[b, :, x] if b % 2 == 0 else sbuf[b, p]
        s1[b] = (kept.astype(F32) + r1[b].astype(F32)).astype(BF16)
        if b % 2 == 0:
            go(s1.at[b, 1 - p], r2.at[b], R_2 + b, ypeer)
        else:
            go(s1.at[b, 1 - x], r2.at[b], R_2 + b, xpeer)

    def stage3(b):
        landed(r2.at[b], R_2 + b)
        kept = s1[b, p] if b % 2 == 0 else s1[b, x]
        cols = pl.ds(pl.multiple_of(where[b] * cut, cut), cut)
        out[:, cols] = (
            mixed[:, cols].astype(F32) + (kept.astype(F32) + r2[b].astype(F32))
        ).astype(BF16)

    stages = (stage0, stage1, stage2, stage3)
    total = 2 * groups
    for step in range(total + 3):
        for i, stage in enumerate(stages):
            if 0 <= step - i < total:
                stage(step - i)

    for cond, one_copy in sends:
        if cond is None:
            one_copy.wait_send()
        else:
            pl.when(cond)(one_copy.wait_send)


def layer(
    sps, tps, residual, queries, keys, values, sinks, out_weight, norm_gain,
    gate_weight, up_weight, down_weight,
):
    rows, width = queries.shape
    own, depth = residual.shape
    blk, ff = gate_weight.shape
    fits = (
        sps % 2 == 0 and 4 <= sps <= 8 and tps == 4 and keys.shape[1] == HEAD
        and blk % 128 == 0 and ff % 32 == 0 and own % 16 == 0
    )
    if not fits:
        return shards(
            residual, queries, keys, values, sinks, out_weight, norm_gain,
            gate_weight, up_weight, down_weight,
        )
    groups, ffh, slots = sps // 2, ff // 2, 2 * tps
    wgu = jnp.concatenate(
        [gate_weight.T.reshape(2, ffh, blk), up_weight.T.reshape(2, ffh, blk)], axis=1
    )
    wd = down_weight.reshape(2, ffh, blk)
    vm = pl.BlockSpec(memory_space=pltpu.VMEM)
    sm = pl.BlockSpec(memory_space=pltpu.SMEM)
    nb = 2 * groups
    return pl.pallas_call(
        functools.partial(whole_layer, sps, tps),
        out_shape=jax.ShapeDtypeStruct((own, depth), BF16),
        in_specs=[vm] * 4 + [sm, pl.BlockSpec(memory_space=pl.ANY)] + [vm] * 3,
        out_specs=vm,
        scratch_shapes=[
            pltpu.VMEM((rows + WINDOW, HEAD), BF16),
            pltpu.VMEM((rows + WINDOW, HEAD), BF16),
            pltpu.VMEM((rows, width), BF16),
            pltpu.VMEM((3, own, width), BF16),
            pltpu.VMEM((own, depth), BF16),
            pltpu.VMEM((slots * own, depth), BF16),
            pltpu.VMEM((groups, 2, 2 * ffh, blk), BF16),
            pltpu.VMEM((groups, 2, ffh, blk), BF16),
            pltpu.VMEM((slots * own, 2 * ffh), F32),
            pltpu.VMEM((slots * own, ffh), BF16),
            pltpu.VMEM((nb, 2, 2, 2, own, blk), BF16),
            pltpu.VMEM((nb, 2, 2, own, blk), BF16),
            pltpu.VMEM((nb, 2, 2, own, blk), BF16),
            pltpu.VMEM((nb, 2, own, blk), BF16),
            pltpu.VMEM((nb, 2, own, blk), BF16),
            pltpu.VMEM((nb, own, blk), BF16),
            pltpu.VMEM(out_weight.shape, BF16),
            pltpu.SemaphoreType.DMA,
            pltpu.SemaphoreType.DMA((24 * groups + 48,)),
            pltpu.SemaphoreType.DMA((24 * groups + 48,)),
        ],
        compiler_params=pltpu.CompilerParams(
            collective_id=0, has_side_effects=True, vmem_limit_bytes=66000000
        ),
        name="whole_layer",
    )(residual, queries, keys, values, sinks, out_weight, norm_gain.reshape(1, depth), wgu, wd)


def solution(mesh):
    placed = (
        P(("sp", "tp"), None),
        P("sp", "tp"),
        P("sp", "tp"),
        P("sp", "tp"),
        P("tp"),
        P(),
        P(),
        P("sp", "tp"),
        P("sp", "tp"),
        P("tp", "sp"),
    )
    return jax.shard_map(
        functools.partial(layer, mesh.shape["sp"], mesh.shape["tp"]), mesh=mesh, in_specs=placed, out_specs=P(("sp", "tp"), None), check_vma=False
    )
```
